32 devices in a mesh: grp: 2 (over y), ep: 4 (over z), tp: 4 (over x, core).
Axes of the slice: x: 2, y: 2, z: 4, core: 2. Of those that a mesh axis runs over, the one named last changes fastest.
Arguments:
- queries: bfloat16 [2048, 1024], P(('grp', 'ep'), 'tp'), parts along dimension 0, may hold values from -6 to 6
- head_key_rows: bfloat16 [2048, 1024], P(('grp', 'ep'), 'tp'), parts along dimension 0, may hold values from -6 to 6
- head_value_rows: bfloat16 [2048, 2048], P(('grp', 'ep'), 'tp'), parts along dimension 0, may hold values from -6 to 6
- output_gate_logits: bfloat16 [2048, 2048], P(('grp', 'ep'), 'tp'), parts along dimension 0, may hold values from -6 to 6
- log_input_gate: float32 [4, 2048], P('tp', ('grp', 'ep')), parts along dimension 1, may hold values from -5 to 103
- forget_gate_logits: float32 [4, 2048], P('tp', ('grp', 'ep')), parts along dimension 1, may hold values from 1 to 20
- extra_log_forget: float32 [4, 2048], P('tp', ('grp', 'ep')), parts along dimension 1, may hold values from -1 to 0, as said below
- head_norm_gain: float32 [2048], P('tp'), may hold values from 0.1 to 1.9
- memory_output_matrix: bfloat16 [2048, 2048], P('tp'), may hold values from -0.125 to 0.125
- expert_input_tokens: bfloat16 [2048, 2048], P(('grp', 'ep', 'tp')), parts along dimension 0, may hold values from -6 to 6
- expert_norm_gain: float32 [2048], replicated, may hold values from 0.1 to 1.9
- routes: int32 [2048, 2], P(('grp', 'ep', 'tp')), parts along dimension 0, may hold values from 0 to 15, all different within a row; in each aligned block of 64 rows (0 to 63, 64 to 127, ...) at most 16 rows name the same one
- routed_expert_weight: float32 [2048, 2], P(('grp', 'ep', 'tp')), parts along dimension 0, may hold values from 0.1 to 1
- expert_gate_matrix: bfloat16 [16, 2048, 512], P(('ep', 'tp')), may hold values from -0.125 to 0.125
- expert_up_matrix: bfloat16 [16, 2048, 512], P(('ep', 'tp')), may hold values from -0.125 to 0.125
- expert_down_matrix: bfloat16 [16, 512, 2048], P(('ep', 'tp')), may hold values from -0.25 to 0.25
Outputs:
- mixer_out: bfloat16 [2048, 2048], P(('grp', 'ep', 'tp')), parts along dimension 0
- expert_out: bfloat16 [2048, 2048], P(('grp', 'ep', 'tp')), parts along dimension 0
The draws below stay inside these ranges and needn't reach their ends.
There are 2 independent parts, one for each index of `grp`. The reference program is written for one: setup_inputs(seed, part) draws one part's arguments, and reference() takes and returns one part's arrays. A program takes and returns all parts, laid end to end along the dimension named above; an argument that names none is the same for every part. Nothing has to cross between parts.
Inputs may be any that keep to these rules, and one draw needn't show every extreme that they name: `routes`: each row names 2 different experts. In the rows of one device (aligned blocks of 64 rows) no expert is named more than 16 times, and in some blocks one expert is named exactly 16 times. `extra_log_forget`: mostly zero.
All inputs are finite; a program needn't handle non-finite values.
Results may differ from the reference program's by a relative error of at most 0.009.
Values may be sent and summed in bfloat16 or wider, within the bound.
A program may use at most 128 MiB of HBM per device.

```python
import math
import jax
import jax.numpy as jnp
import numpy as np
from jax import lax

D = 2048
HEADS = 4
DQK = 256
DV = 512
FE = 512
TOP = 2
TOKB_DEV = 64
EXPERTS = 16
SPAN = 256
SEQ_A = 1024
TOKENS_B = 1024
CAP = 16
N_EP = 4
N_TP = 4


def draw_log_input_gate(key, part):
    drawn = jax.random.uniform(key, (HEADS, SEQ_A), jnp.float32, -5.0, 3.0)
    return drawn


def draw_forget_gate_logits(key, part):
    order_key = jax.random.fold_in(key, 11)
    shift_key = jax.random.fold_in(key, 12)
    noise_key = jax.random.fold_in(key, 13)
    head_order = jax.random.permutation(order_key, HEADS)
    head_rank = jnp.argsort(head_order)
    fast_count = HEADS // 2
    slow_base = math.log(SEQ_A) + 1.0
    base_level = jnp.where(head_rank < fast_count, 3.5, slow_base).astype(jnp.float32)
    block_shift = jax.random.uniform(shift_key, (HEADS, SEQ_A // SPAN), jnp.float32, -0.8, 0.8)
    block_shift = jnp.repeat(block_shift, SPAN, axis=1)
    noise = jax.random.uniform(noise_key, (HEADS, SEQ_A), jnp.float32, -1.0, 1.0)
    return base_level[:, None] + block_shift + noise


def draw_extra_log_forget(key, part):
    spot_key = jax.random.fold_in(key, 21)
    drop_key = jax.random.fold_in(key, 22)
    spots = jax.random.randint(spot_key, (HEADS, 3), 0, SEQ_A)
    drops = jax.random.uniform(drop_key, (HEADS, 3), jnp.float32, -0.5, -0.22)
    places = jnp.arange(SEQ_A)[None, None, :] == spots[:, :, None]
    return jnp.sum(jnp.where(places, drops[:, :, None], 0.0), axis=1).astype(jnp.float32)


def block_levels(stream_key, extent, split, least, top_value):
    loudness = 1.0
    for axis_at, parts in split:
        draws = jax.random.uniform(jax.random.fold_in(jax.random.fold_in(stream_key, 6), axis_at), (parts,), jnp.float32, least / len(split), top_value / len(split))
        loudness = loudness * jnp.repeat(jnp.exp(draws), extent[axis_at] // parts).reshape((-1,) + (1,) * (len(extent) - 1 - axis_at))
    return loudness


def routed_block(key, own, number, rows, number_of, top, most, lean):
    order = jax.random.permutation(key, number_of)
    packed, usual = shares(number_of, rows * top, most, lean, True), shares(number_of, rows * top, most, lean, False)
    places = jnp.arange(number_of)

    def named(lengths, offset_by):
        used = int((lengths > 0).sum())
        fixed = max(1, used // 4)
        passed = fixed + (places - fixed + offset_by * (used - fixed)) % max(1, number_of - fixed)
        return jnp.zeros((number_of,), jnp.int32).at[order[jnp.where(places < fixed, places, passed)]].set(jnp.asarray(lengths, jnp.int32))

    lengths = jnp.where(number % 4 == 0, named(packed, number // 4), named(usual, number - number // 4 - 1))
    mixed = jax.random.permutation(jax.random.fold_in(own, 3), number_of)
    donor, receiver = mixed[0:number_of // 2 * 2:2], mixed[1:number_of // 2 * 2:2]
    slack = jnp.minimum(lengths[donor] - 1, most - lengths[receiver]) // 2
    slack = jnp.where((donor == order[0]) | (receiver == order[0]) | (lengths[receiver] == 0), 0, jnp.maximum(slack, 0))
    passed = jax.random.randint(jax.random.fold_in(own, 4), (number_of // 2,), 0, 1 << 20) % (slack + 1)
    lengths = lengths.at[donor].add(-passed).at[receiver].add(passed)
    items = jnp.searchsorted(jnp.cumsum(lengths), jnp.arange(rows * top), side="right").astype(jnp.int32)
    table = items.reshape(top, rows).T
    table = table[jax.random.permutation(jax.random.fold_in(own, 1), rows)]
    offset_by = jax.random.randint(jax.random.fold_in(own, 2), (rows, 1), 0, top)
    return jnp.take_along_axis(table, (jnp.arange(top)[None, :] + offset_by) % top, axis=1)


def shares(number_of, total, most, slope, full):
    loads = [(1 << 20) // math.isqrt(standing ** slope) + 1 for standing in range(1, number_of + 1)]
    largest = most if full else min(most, max(-(-total // number_of), total * loads[0] // sum(loads)))
    least = 1 if total - largest >= number_of - 1 else 0
    holding, rest = [largest] + [least] * (number_of - 1), total - largest - least * (number_of - 1)
    while rest > 0:
        movable = [i for i in range(1, number_of) if holding[i] < largest] or [i for i in range(1, number_of) if holding[i] < most]
        mass, remaining = sum([loads[i] for i in movable]), rest
        for i in movable:
            more = min(most - holding[i], max(1, remaining * loads[i] // mass), rest)
            holding[i] = holding[i] + more
            rest = rest - more
    return np.array(holding)


def gaussian(stream_key, dims, scale, limit, shards=(), kind=jnp.bfloat16):
    loudness = block_levels(stream_key, dims, shards, -0.22, 0.18) if shards else 1.0
    result = jax.random.normal(stream_key, dims, jnp.float32) * scale * loudness
    return jnp.minimum(jnp.maximum(result, -limit), limit).astype(kind)


def setup_inputs(seed: int = 0, part: int = 0) -> dict:
    splits = jax.random.split(jax.random.key(seed), 17)
    part_keys = jax.random.split(jax.random.fold_in(splits[16], part), 17)
    queries = gaussian(part_keys[0], (SEQ_A, HEADS * DQK), 1.0, 6.0, ((0, 4), (1, 4)))
    head_key_rows = gaussian(part_keys[1], (SEQ_A, HEADS * DQK), 1.0, 6.0, ((0, 4), (1, 4)))
    head_value_rows = gaussian(part_keys[2], (SEQ_A, HEADS * DV), 1.0, 6.0, ((0, 4), (1, 4)))
    output_gate_logits = gaussian(part_keys[3], (SEQ_A, HEADS * DV), 1.0, 6.0, ((0, 4), (1, 4)))
    log_input_gate = draw_log_input_gate(jax.random.fold_in(jax.random.fold_in(splits[16], part), 71), part)
    forget_gate_logits = draw_forget_gate_logits(jax.random.fold_in(jax.random.fold_in(splits[16], part), 71), part)
    extra_log_forget = draw_extra_log_forget(jax.random.fold_in(jax.random.fold_in(splits[16], part), 71), part)
    head_norm_gain = jnp.clip(1.0 + 0.18 * jax.random.normal(splits[7], (HEADS * DV,), jnp.float32), 0.1, 1.9)
    memory_output_matrix = gaussian(splits[8], (HEADS * DV, D), (HEADS * DV) ** -0.5, 0.125, ((0, 4),))
    expert_input_tokens = gaussian(part_keys[9], (TOKENS_B, D), 1.0, 6.0, ((0, 16),))
    expert_norm_gain = jnp.clip(1.0 + 0.18 * jax.random.normal(splits[10], (D,), jnp.float32), 0.1, 1.9)
    routes_keys = jax.random.split(jax.random.fold_in(part_keys[11], 1), TOKENS_B // TOKB_DEV)
    routes_turns = jax.random.permutation(jax.random.fold_in(part_keys[11], 3), TOKENS_B // TOKB_DEV)
    routes = jax.vmap(lambda own, number: routed_block(jax.random.fold_in(part_keys[11], 2), own, number, TOKB_DEV, EXPERTS, TOP, CAP, 1))(routes_keys, routes_turns).reshape((TOKENS_B, TOP))
    routed_expert_weight = jnp.clip(0.1 + 0.9 * jax.random.uniform(part_keys[12], (TOKENS_B, TOP), jnp.float32) ** block_levels(part_keys[12], (TOKENS_B, TOP), ((0, 16),), -0.2, 0.2), 0.1, 1.0)
    expert_gate_matrix = gaussian(splits[13], (EXPERTS, D, FE), D ** -0.5, 0.125, ((0, 16),))
    expert_up_matrix = gaussian(splits[14], (EXPERTS, D, FE), D ** -0.5, 0.125, ((0, 16),))
    expert_down_matrix = gaussian(splits[15], (EXPERTS, FE, D), FE ** -0.5, 0.25, ((0, 16),))
    return {"queries": queries, "head_key_rows": head_key_rows, "head_value_rows": head_value_rows, "output_gate_logits": output_gate_logits, "log_input_gate": log_input_gate, "forget_gate_logits": forget_gate_logits, "extra_log_forget": extra_log_forget, "head_norm_gain": head_norm_gain, "memory_output_matrix": memory_output_matrix, "expert_input_tokens": expert_input_tokens, "expert_norm_gain": expert_norm_gain, "routes": routes, "routed_expert_weight": routed_expert_weight, "expert_gate_matrix": expert_gate_matrix, "expert_up_matrix": expert_up_matrix, "expert_down_matrix": expert_down_matrix}


lowest_log = -1e+30
norm_eps = 1e-06
layer_eps = 1e-05

def join_states(earlier, later):
    early_memory, early_top, early_total = earlier
    late_memory, late_top, late_total = later
    joined_top = jnp.maximum(late_total + early_top, late_top)
    joined_memory = jnp.exp(late_total + early_top - joined_top) * early_memory + jnp.exp(late_top - joined_top) * late_memory
    return (joined_memory, joined_top, early_total + late_total)

def block_summary(keys_f32, values_f32, log_weight):
    top_weight = jnp.max(log_weight)
    weighted = keys_f32 * jnp.exp(log_weight - top_weight)[:, None]
    memory = jnp.einsum('sd,se->de', weighted, values_f32, precision=lax.Precision.HIGHEST)
    return (memory, top_weight)

def block_output(queries, head_key_rows, head_value_rows, output_gate_logits, in_gate, through, before, span_total, prior_memory, prior_top, later_memory, later_top, head_norm_gain):
    score_scale = queries.shape[1] ** (-0.5)
    from_prior = through + prior_top
    from_later = span_total - before + later_top
    fw_log = through[:, None] - through[None, :] + in_gate[None, :]
    bw_log = before[None, :] - before[:, None] + in_gate[None, :]
    positions = jnp.arange(queries.shape[0])
    lower_mask = positions[:, None] >= positions[None, :]
    upper_mask = positions[:, None] <= positions[None, :]
    inner_top = jnp.maximum(lax.optimization_barrier(jnp.max(jnp.where(lower_mask, fw_log, -jnp.inf), axis=1)), lax.optimization_barrier(jnp.max(jnp.where(upper_mask, bw_log, -jnp.inf), axis=1)))
    row_top = jnp.maximum(inner_top, jnp.maximum(from_prior, from_later))
    weights = jnp.where(lower_mask, jnp.exp(fw_log - row_top[:, None]), 0.0) + jnp.where(upper_mask, jnp.exp(bw_log - row_top[:, None]), 0.0)
    scores = jnp.einsum('td,sd->ts', queries, head_key_rows, preferred_element_type=jnp.float32) * score_scale
    near_weights = (scores * weights).astype(jnp.bfloat16)
    queries_f32 = queries.astype(jnp.float32)
    carried = jnp.exp(from_prior - row_top)[:, None] * jnp.dot(queries_f32, prior_memory, precision=lax.Precision.HIGHEST)
    carried = carried + jnp.exp(from_later - row_top)[:, None] * jnp.dot(queries_f32, later_memory, precision=lax.Precision.HIGHEST)
    head_rows = jnp.dot(near_weights, head_value_rows, preferred_element_type=jnp.float32) + carried * score_scale
    normed = head_rows * lax.rsqrt(lax.optimization_barrier(jnp.mean(head_rows * head_rows, axis=1, keepdims=True)) + norm_eps) * head_norm_gain
    return (jax.nn.sigmoid(output_gate_logits.astype(jnp.float32)) * normed).astype(jnp.bfloat16)

def mixer_head(queries, head_key_rows, head_value_rows, output_gate_logits, in_gate, forget_log_value, head_norm_gain):
    blocks = queries.shape[0] // SPAN

    def split_rows(stacked):
        return stacked.reshape((blocks, SPAN) + stacked.shape[1:])
    query_blocks = split_rows(queries)
    key_blocks = split_rows(head_key_rows)
    value_blocks = split_rows(head_value_rows)
    gate_blocks = split_rows(output_gate_logits)
    input_blocks = split_rows(in_gate)
    forget_blocks = split_rows(forget_log_value)
    through = jnp.cumsum(forget_blocks, axis=1)
    before = through - forget_blocks
    span_total = through[:, -1]
    keys_f32 = key_blocks.astype(jnp.float32)
    values_f32 = value_blocks.astype(jnp.float32)
    fw_memory, fw_top = jax.vmap(block_summary)(keys_f32, values_f32, span_total[:, None] - through + input_blocks)
    bw_memory, bw_top = jax.vmap(block_summary)(keys_f32, values_f32, before + input_blocks)
    identity = (jnp.zeros((DQK, DV), jnp.float32), jnp.array(lowest_log, jnp.float32), jnp.array(0.0, jnp.float32))

    def chain_step(running, element):
        return (join_states(running, element), running)
    _, prior_carry = lax.scan(chain_step, identity, (fw_memory, fw_top, span_total))
    _, later_carry = lax.scan(chain_step, identity, (bw_memory, bw_top, span_total), reverse=True)

    def one_block(pieces):
        return block_output(*pieces, head_norm_gain)
    gated_rows = lax.map(one_block, (query_blocks, key_blocks, value_blocks, gate_blocks, input_blocks, through, before, span_total, prior_carry[0], prior_carry[1], later_carry[0], later_carry[1]))
    return gated_rows.reshape(blocks * SPAN, DV)

def expert_half(expert_input_tokens, expert_norm_gain, routes, routed_expert_weight, expert_gate_matrix, expert_up_matrix, expert_down_matrix):
    tokens_f32 = expert_input_tokens.astype(jnp.float32)
    centre = lax.optimization_barrier(jnp.mean(tokens_f32, axis=1, keepdims=True))
    spread = lax.optimization_barrier(jnp.mean(jnp.square(tokens_f32 - centre), axis=1, keepdims=True))
    normed = ((tokens_f32 - centre) * lax.rsqrt(spread + layer_eps) * expert_norm_gain).astype(jnp.bfloat16)
    token_count = expert_input_tokens.shape[0]
    flat_expert = routes.reshape(-1).astype(jnp.int32)
    flat_weight = routed_expert_weight.reshape(-1)
    pair_order = jnp.argsort(flat_expert, stable=True).astype(jnp.int32)
    sorted_expert = flat_expert[pair_order]
    counts = lax.optimization_barrier(jnp.sum((flat_expert[None, :] == jnp.arange(EXPERTS, dtype=jnp.int32)[:, None]).astype(jnp.int32), axis=1))
    starts = (jnp.cumsum(counts) - counts).astype(jnp.int32)
    most_rows = CAP * N_EP * N_TP
    padded_order = jnp.concatenate([pair_order, jnp.zeros((most_rows,), jnp.int32)])
    padded_expert = jnp.concatenate([sorted_expert, jnp.full((most_rows,), -1, jnp.int32)])

    def one_expert(output_sum, expert):
        first = starts[expert].astype(jnp.int32)
        pair_index = lax.dynamic_slice(padded_order, (first,), (most_rows,))
        live_slot = (lax.dynamic_slice(padded_expert, (first,), (most_rows,)) == expert).astype(jnp.float32)
        token_rows = (pair_index // TOP).astype(jnp.int32)
        picked = normed[token_rows]
        gate_part = jnp.dot(picked, expert_gate_matrix[expert], preferred_element_type=jnp.float32)
        up_part = jnp.dot(picked, expert_up_matrix[expert], preferred_element_type=jnp.float32)
        hidden = (jax.nn.silu(gate_part) * up_part).astype(jnp.bfloat16)
        expert_rows = jnp.dot(hidden, expert_down_matrix[expert], preferred_element_type=jnp.float32).astype(jnp.bfloat16)
        expert_rows = lax.optimization_barrier(expert_rows).astype(jnp.float32)
        scaled = (flat_weight[pair_index] * live_slot)[:, None] * expert_rows
        return (output_sum.at[token_rows].add(scaled), None)
    output_sum, _ = lax.scan(one_expert, jnp.zeros((token_count, D), jnp.float32), jnp.arange(EXPERTS, dtype=jnp.int32))
    return output_sum.astype(jnp.bfloat16)

def reference(queries, head_key_rows, head_value_rows, output_gate_logits, log_input_gate, forget_gate_logits, extra_log_forget, head_norm_gain, memory_output_matrix, expert_input_tokens, expert_norm_gain, routes, routed_expert_weight, expert_gate_matrix, expert_up_matrix, expert_down_matrix):
    forget_log_value = jax.nn.log_sigmoid(forget_gate_logits) + extra_log_forget
    mixed_sum = jnp.zeros((queries.shape[0], D), jnp.float32)
    for head_index in range(HEADS):
        gated_rows = mixer_head(queries[:, head_index * DQK:(head_index + 1) * DQK], head_key_rows[:, head_index * DQK:(head_index + 1) * DQK], head_value_rows[:, head_index * DV:(head_index + 1) * DV], output_gate_logits[:, head_index * DV:(head_index + 1) * DV], log_input_gate[head_index], forget_log_value[head_index], head_norm_gain[head_index * DV:(head_index + 1) * DV])
        head_part = jnp.dot(gated_rows, memory_output_matrix[head_index * DV:(head_index + 1) * DV], preferred_element_type=jnp.float32).astype(jnp.bfloat16)
        mixed_sum = mixed_sum + lax.optimization_barrier(head_part).astype(jnp.float32)
    expert_out = expert_half(expert_input_tokens, expert_norm_gain, routes, routed_expert_weight, expert_gate_matrix, expert_up_matrix, expert_down_matrix)
    return (mixed_sum.astype(jnp.bfloat16), expert_out)
```

```python
import functools

import jax
import jax.numpy as jnp
from jax import lax
from jax.experimental import pallas as pl
from jax.experimental.pallas import tpu as pltpu
from jax.sharding import PartitionSpec as P

lowest_log = -1e30
norm_eps = 1e-06
layer_eps = 1e-05
row_tile = 16

F32 = jnp.float32
BF16 = jnp.bfloat16


def dot(a, b, contract=((1,), (0,))):
    return lax.dot_general(a, b, (contract, ((), ())), preferred_element_type=F32)


def step_kernel(
    ep,
    tp,
    stride,
    capacity,
    q_ref,
    k_ref,
    v_ref,
    og_ref,
    ig_ref,
    fg_ref,
    xf_ref,
    hgain_ref,
    wo_hbm,
    tok_ref,
    egain_ref,
    routes_ref,
    rw_ref,
    wg_hbm,
    wu_hbm,
    wd_hbm,
    mix_ref,
    exp_ref,
    wo,
    wg,
    wu,
    wd,
    out_rows,
    arrived,
    results,
    returned,
    comb,
    fw_own,
    bw_own,
    fw_in,
    bw_in,
    fw_out,
    bw_out,
    fw_top_in,
    bw_top_in,
    fw_top_out,
    bw_top_out,
    parts_out,
    parts_in,
    gated,
    hidden,
    w_sem,
    d_send,
    d_recv,
    r_send,
    r_recv,
    c_send,
    c_recv,
    p_send,
    p_recv,
):
    n = ep * tp
    z = lax.axis_index("ep")
    t = lax.axis_index("tp")
    me = z * tp + t
    span = q_ref.shape[0]
    tokens, width = tok_ref.shape
    sub = span // tp

    def peer(dz, dt):
        return lax.rem(z + dz, ep), lax.rem(t + dt, tp)

    def to(z2, t2):
        return {"ep": z2, "tp": t2}

    barrier = pltpu.get_barrier_semaphore()

    def greet(i, c):
        z2, t2 = peer(i // tp, lax.rem(i, tp))
        pl.semaphore_signal(
            barrier, inc=1, device_id=to(z2, t2), device_id_type=pl.DeviceIdType.MESH
        )
        return c

    lax.fori_loop(1, n, greet, 0)

    loads = [
        pltpu.make_async_copy(src, dst, w_sem.at[i])
        for i, (src, dst) in enumerate(
            ((wo_hbm, wo), (wg_hbm.at[0], wg), (wu_hbm.at[0], wu), (wd_hbm.at[0], wd))
        )
    ]
    for load in loads:
        load.start()

    rows_i = lax.broadcasted_iota(jnp.int32, (span, span), 0)
    cols_i = lax.broadcasted_iota(jnp.int32, (span, span), 1)
    lower = rows_i >= cols_i
    upper = rows_i <= cols_i
    diag = rows_i == cols_i

    fg = fg_ref[...]
    lf_row = jnp.minimum(fg, 0.0) - jnp.log1p(jnp.exp(-jnp.abs(fg))) + xf_ref[...]
    in_row = ig_ref[...]
    lf_col = jnp.sum(jnp.where(diag, lf_row, 0.0), axis=1, keepdims=True)
    in_col = jnp.sum(jnp.where(diag, in_row, 0.0), axis=1, keepdims=True)
    through_col = jnp.sum(jnp.where(lower, lf_row, 0.0), axis=1, keepdims=True)
    through_row = jnp.sum(jnp.where(upper, lf_col, 0.0), axis=0, keepdims=True)
    before_col = through_col - lf_col
    before_row = through_row - lf_row
    total = jnp.sum(lf_row, axis=1, keepdims=True)

    keys = k_ref[...]
    values = v_ref[...]
    keys_f32 = keys.astype(F32)
    fw_w = total - through_col + in_col
    bw_w = before_col + in_col
    fw_top = jnp.max(fw_w, axis=0, keepdims=True)
    bw_top = jnp.max(bw_w, axis=0, keepdims=True)
    fw_own[...] = dot((keys_f32 * jnp.exp(fw_w - fw_top)).astype(BF16), values, ((0,), (0,)))
    bw_own[...] = dot((keys_f32 * jnp.exp(bw_w - bw_top)).astype(BF16), values, ((0,), (0,)))

    x = tok_ref[...].astype(F32)
    centre = jnp.mean(x, axis=1, keepdims=True)
    spread = jnp.mean(jnp.square(x - centre), axis=1, keepdims=True)
    normed = ((x - centre) * lax.rsqrt(spread + layer_eps) * egain_ref[...]).astype(BF16)
    routes = routes_ref[...]
    lanes = max(128, -(-n // 128) * 128)
    lane_e = lax.broadcasted_iota(jnp.int32, (tokens, lanes), 1)
    top = routes.shape[1]
    hots = [(lane_e == routes[:, i : i + 1]).astype(F32) for i in range(top)]
    tok_r = lax.broadcasted_iota(jnp.int32, (tokens, tokens), 0)
    tok_c = lax.broadcasted_iota(jnp.int32, (tokens, tokens), 1)
    earlier = dot((tok_r > tok_c).astype(F32).astype(BF16), sum(hots).astype(BF16))
    slot_i = lax.broadcasted_iota(jnp.int32, (tokens, n * stride), 1)
    pick = jnp.zeros((tokens, n * stride), F32)
    weigh = jnp.zeros((tokens, n * stride), F32)
    for i in range(top):
        place = jnp.sum(earlier * hots[i], axis=1, keepdims=True).astype(jnp.int32)
        mine = (slot_i == routes[:, i : i + 1] * stride + place).astype(F32)
        pick = pick + mine
        weigh = weigh + mine * rw_ref[:, i : i + 1]
    comb[...] = weigh
    pick = pick.astype(BF16)
    out_rows[...] = dot(pick, normed, ((0,), (0,))).astype(BF16)

    pl.semaphore_wait(barrier, n - 1)

    def rows_of(ref, index):
        return ref.at[pl.ds(pl.multiple_of(index * stride, row_tile), stride)]

    def exchange(src, dst, send, recv, z2, t2, arriving):
        p = z2 * tp + t2
        return pltpu.make_async_remote_copy(
            src_ref=rows_of(src, p),
            dst_ref=rows_of(dst, p if arriving else me),
            send_sem=send.at[p],
            recv_sem=recv.at[p if arriving else me],
            device_id=to(z2, t2),
            device_id_type=pl.DeviceIdType.MESH,
        )

    def dispatch(z2, t2, arriving=False):
        return exchange(out_rows, arrived, d_send, d_recv, z2, t2, arriving)

    def give_back(z2, t2, arriving=False):
        return exchange(results, returned, r_send, r_recv, z2, t2, arriving)

    def each_peer(first, action):
        def turn(i, c):
            z2, t2 = peer(i // tp, lax.rem(i, tp))
            action(z2, t2)
            return c

        lax.fori_loop(first, n, turn, 0)

    own = pl.ds(pl.multiple_of(me * stride, row_tile), stride)

    def chain(index, src, dst, z2):
        return pltpu.make_async_remote_copy(
            src_ref=src,
            dst_ref=dst,
            send_sem=c_send.at[index],
            recv_sem=c_recv.at[index],
            device_id=to(z2, t),
            device_id_type=pl.DeviceIdType.MESH,
        )

    after = lax.rem(z + 1, ep)
    ahead = lax.rem(z + ep - 1, ep)
    fw_chain = (chain(0, fw_top_out, fw_top_in, after), chain(1, fw_out, fw_in, after))
    bw_chain = (chain(2, bw_top_out, bw_top_in, ahead), chain(3, bw_out, bw_in, ahead))

    @pl.when(z == 0)
    def _():
        fw_in[...] = jnp.zeros_like(fw_in)
        fw_top_in[...] = jnp.full_like(fw_top_in, lowest_log)

    @pl.when(z == ep - 1)
    def _():
        bw_in[...] = jnp.zeros_like(bw_in)
        bw_top_in[...] = jnp.full_like(bw_top_in, lowest_log)

    def pass_on(copies, in_ref, top_in, own_ref, own_top, out_ref, top_out):
        shifted = total + top_in[0:1, 0:1]
        joined = jnp.maximum(shifted, own_top)
        out_ref[...] = (
            jnp.exp(shifted - joined) * in_ref[...].astype(F32)
            + jnp.exp(own_top - joined) * own_ref[...]
        ).astype(BF16)
        top_out[...] = jnp.broadcast_to(joined, top_out.shape)
        for copy in copies:
            copy.start()

    def stage(s, c):
        @pl.when(z == s)
        def _():
            @pl.when(z > 0)
            def _():
                for copy in fw_chain:
                    copy.wait_recv()

            pass_on(fw_chain, fw_in, fw_top_in, fw_own, fw_top, fw_out, fw_top_out)

        @pl.when(ep - 1 - z == s)
        def _():
            @pl.when(z < ep - 1)
            def _():
                for copy in bw_chain:
                    copy.wait_recv()

            pass_on(bw_chain, bw_in, bw_top_in, bw_own, bw_top, bw_out, bw_top_out)

        def plane(dt, c2):
            z2, t2 = peer(s + 1, dt)
            dispatch(z2, t2).start()
            return c2

        return lax.fori_loop(0, tp, plane, c)

    def near_plane(dt, c):
        z2, t2 = peer(0, dt)
        dispatch(z2, t2).start()
        return c

    lax.fori_loop(1, tp, near_plane, 0)
    lax.fori_loop(0, ep - 1, stage, 0)
    arrived[own] = out_rows[own]

    from_row = through_col - through_row + in_row
    fw_log = jnp.where(lower, from_row, -jnp.inf)
    bw_log = jnp.where(upper, before_row - before_col + in_row, -jnp.inf)
    inner_top = jnp.maximum(
        jnp.max(fw_log, axis=1, keepdims=True), jnp.max(bw_log, axis=1, keepdims=True)
    )

    @pl.when(z == ep - 1)
    def _():
        for copy in fw_chain:
            copy.wait_recv()

    @pl.when(z == 0)
    def _():
        for copy in bw_chain:
            copy.wait_recv()

    from_prior = through_col + fw_top_in[0:1, 0:1]
    from_later = total - before_col + bw_top_in[0:1, 0:1]
    row_top = jnp.maximum(inner_top, jnp.maximum(from_prior, from_later))
    weights = jnp.exp(fw_log - row_top) + jnp.exp(bw_log - row_top)
    queries = q_ref[...]
    scale = queries.shape[1] ** (-0.5)
    scores = dot(queries, keys, ((1,), (1,))) * scale
    near = (scores * weights).astype(BF16)
    carried = jnp.exp(from_prior - row_top) * dot(queries, fw_in[...])
    carried = carried + jnp.exp(from_later - row_top) * dot(queries, bw_in[...])
    head_rows = dot(near, values) + carried * scale
    mean_square = jnp.mean(head_rows * head_rows, axis=1, keepdims=True)
    normed_rows = head_rows * lax.rsqrt(mean_square + norm_eps) * hgain_ref[...]
    gated[...] = (jax.nn.sigmoid(og_ref[...].astype(F32)) * normed_rows).astype(BF16)

    loads[0].wait()
    cols = 256

    def project(i, c):
        at = pl.ds(pl.multiple_of(i * cols, cols), cols)
        parts_out[:, at] = dot(gated[...], wo[:, at]).astype(BF16)
        return c

    lax.fori_loop(0, width // cols, project, 0)

    def share(dt, arriving=False):
        t2 = lax.rem(t + dt, tp)
        slot = t2 if arriving else t
        return pltpu.make_async_remote_copy(
            src_ref=parts_out.at[pl.ds(pl.multiple_of(t2 * sub, row_tile), sub)],
            dst_ref=parts_in.at[slot],
            send_sem=p_send.at[t2],
            recv_sem=p_recv.at[slot],
            device_id=to(z, t2),
            device_id_type=pl.DeviceIdType.MESH,
        )

    for dt in range(1, tp):
        share(dt).start()
    parts_in[t] = parts_out[pl.ds(pl.multiple_of(t * sub, row_tile), sub), :]

    for load in loads[1:]:
        load.wait()
    each_peer(1, lambda z2, t2: dispatch(z2, t2, True).wait_recv())
    fe = wg.shape[1]
    chunk = min(256, n * stride)

    def expert_chunk(i, c):
        at = pl.ds(pl.multiple_of(i * chunk, chunk), chunk)

        def up(j, c2):
            f = pl.ds(pl.multiple_of(j * cols, cols), cols)
            rows = arrived[at, :]
            gate_part = dot(rows, wg[:, f])
            up_part = dot(rows, wu[:, f])
            hidden[:, f] = (gate_part * jax.nn.sigmoid(gate_part) * up_part).astype(BF16)
            return c2

        lax.fori_loop(0, fe // cols, up, 0)

        def down(j, c2):
            f = pl.ds(pl.multiple_of(j * cols, cols), cols)
            results[at, f] = dot(hidden[...], wd[:, f]).astype(BF16)
            return c2

        return lax.fori_loop(0, width // cols, down, c)

    lax.fori_loop(0, n * stride // chunk, expert_chunk, 0)
    each_peer(1, lambda z2, t2: give_back(z2, t2).start())
    returned[own] = results[own]

    for dt in range(1, tp):
        share(dt, True).wait_recv()
    mixed = parts_in[0].astype(F32)
    for i in range(1, tp):
        mixed = mixed + parts_in[i].astype(F32)
    mix_ref[...] = mixed.astype(BF16)

    weigh = comb[...]
    high = weigh.astype(BF16)
    low = (weigh - high.astype(F32)).astype(BF16)
    each_peer(1, lambda z2, t2: give_back(z2, t2, True).wait_recv())
    for j in range(width // cols):
        f = slice(j * cols, (j + 1) * cols)
        rows = returned[:, f]
        exp_ref[:, f] = (dot(high, rows) + dot(low, rows)).astype(BF16)

    @pl.when(z < ep - 1)
    def _():
        for copy in fw_chain:
            copy.wait_send()

    @pl.when(z > 0)
    def _():
        for copy in bw_chain:
            copy.wait_send()

    for dt in range(1, tp):
        share(dt).wait_send()
    each_peer(1, lambda z2, t2: dispatch(z2, t2).wait_send())
    each_peer(1, lambda z2, t2: give_back(z2, t2).wait_send())


def body(
    queries,
    head_key_rows,
    head_value_rows,
    output_gate_logits,
    log_input_gate,
    forget_gate_logits,
    extra_log_forget,
    head_norm_gain,
    memory_output_matrix,
    expert_input_tokens,
    expert_norm_gain,
    routes,
    routed_expert_weight,
    expert_gate_matrix,
    expert_up_matrix,
    expert_down_matrix,
):
    ep = lax.axis_size("ep")
    tp = lax.axis_size("tp")
    n = ep * tp
    span, dqk = queries.shape
    dv = head_value_rows.shape[1]
    tokens, width = expert_input_tokens.shape
    fe = expert_gate_matrix.shape[2]
    capacity = max(2, 2 * tokens * routes.shape[1] // n)
    stride = -(-capacity // row_tile) * row_tile
    slots = n * stride
    vmem = pl.BlockSpec(memory_space=pltpu.VMEM)
    hbm = pl.BlockSpec(memory_space=pl.ANY)
    dma = pltpu.SemaphoreType.DMA
    return pl.pallas_call(
        functools.partial(step_kernel, ep, tp, stride, capacity),
        out_shape=(
            jax.ShapeDtypeStruct((span // tp, width), BF16),
            jax.ShapeDtypeStruct((tokens, width), BF16),
        ),
        in_specs=[vmem] * 8 + [hbm] + [vmem] * 4 + [hbm] * 3,
        out_specs=(vmem, vmem),
        scratch_shapes=[
            pltpu.VMEM((dv, width), BF16),
            pltpu.VMEM((width, fe), BF16),
            pltpu.VMEM((width, fe), BF16),
            pltpu.VMEM((fe, width), BF16),
            pltpu.VMEM((slots, width), BF16),
            pltpu.VMEM((slots, width), BF16),
            pltpu.VMEM((slots, width), BF16),
            pltpu.VMEM((slots, width), BF16),
            pltpu.VMEM((tokens, slots), F32),
            pltpu.VMEM((dqk, dv), F32),
            pltpu.VMEM((dqk, dv), F32),
            pltpu.VMEM((dqk, dv), BF16),
            pltpu.VMEM((dqk, dv), BF16),
            pltpu.VMEM((dqk, dv), BF16),
            pltpu.VMEM((dqk, dv), BF16),
            pltpu.VMEM((8, 128), F32),
            pltpu.VMEM((8, 128), F32),
            pltpu.VMEM((8, 128), F32),
            pltpu.VMEM((8, 128), F32),
            pltpu.VMEM((span, width), BF16),
            pltpu.VMEM((tp, span // tp, width), BF16),
            pltpu.VMEM((span, dv), BF16),
            pltpu.VMEM((min(256, slots), fe), BF16),
            dma((4,)),
            dma((n,)),
            dma((n,)),
            dma((n,)),
            dma((n,)),
            dma((4,)),
            dma((4,)),
            dma((tp,)),
            dma((tp,)),
        ],
        compiler_params=pltpu.CompilerParams(
            collective_id=0, has_side_effects=True, vmem_limit_bytes=64 * 1024 * 1024 - 65536
        ),
    )(
        queries,
        head_key_rows,
        head_value_rows,
        output_gate_logits,
        log_input_gate,
        forget_gate_logits,
        extra_log_forget,
        head_norm_gain[None, :],
        memory_output_matrix,
        expert_input_tokens,
        expert_norm_gain[None, :],
        routes,
        routed_expert_weight,
        expert_gate_matrix,
        expert_up_matrix,
        expert_down_matrix,
    )


def solution(mesh):
    in_specs = (
        P(("grp", "ep"), "tp"),
        P(("grp", "ep"), "tp"),
        P(("grp", "ep"), "tp"),
        P(("grp", "ep"), "tp"),
        P("tp", ("grp", "ep")),
        P("tp", ("grp", "ep")),
        P("tp", ("grp", "ep")),
        P("tp"),
        P("tp", None),
        P(("grp", "ep", "tp"), None),
        P(),
        P(("grp", "ep", "tp"), None),
        P(("grp", "ep", "tp"), None),
        P(("ep", "tp"), None, None),
        P(("ep", "tp"), None, None),
        P(("ep", "tp"), None, None),
    )
    out_specs = (P(("grp", "ep", "tp"), None), P(("grp", "ep", "tp"), None))
    return jax.shard_map(body, mesh=mesh, in_specs=in_specs, out_specs=out_specs, check_vma=False)
```

```python
import functools

import jax
import jax.numpy as jnp
from jax import lax
from jax.experimental import pallas as pl
from jax.experimental.pallas import tpu as pltpu
from jax.sharding import PartitionSpec as P

lowest_log = -1e30
norm_eps = 1e-06
layer_eps = 1e-05
row_tile = 16

F32 = jnp.float32
BF16 = jnp.bfloat16


def dot(a, b, contract=((1,), (0,))):
    return lax.dot_general(a, b, (contract, ((), ())), preferred_element_type=F32)


def step_kernel(
    ep,
    tp,
    stride,
    capacity,
    q_ref,
    k_ref,
    v_ref,
    og_ref,
    ig_ref,
    fg_ref,
    xf_ref,
    hgain_ref,
    wo_hbm,
    tok_ref,
    egain_ref,
    routes_ref,
    rw_ref,
    wg_hbm,
    wu_hbm,
    wd_hbm,
    mix_ref,
    exp_ref,
    wo,
    wg,
    wu,
    wd,
    out_rows,
    arrived,
    results,
    returned,
    comb,
    fw_own,
    bw_own,
    fw_in,
    bw_in,
    fw_out,
    bw_out,
    fw_top_in,
    bw_top_in,
    fw_top_out,
    bw_top_out,
    parts_out,
    parts_in,
    gated,
    hidden,
    w_sem,
    d_send,
    d_recv,
    r_send,
    r_recv,
    c_send,
    c_recv,
    p_send,
    p_recv,
):
    n = ep * tp
    z = lax.axis_index("ep")
    t = lax.axis_index("tp")
    me = z * tp + t
    span = q_ref.shape[0]
    tokens, width = tok_ref.shape
    sub = span // tp

    def peer(dz, dt):
        return lax.rem(z + dz, ep), lax.rem(t + dt, tp)

    def to(z2, t2):
        return {"ep": z2, "tp": t2}

    barrier = pltpu.get_barrier_semaphore()

    def greet(i, c):
        z2, t2 = peer(i // tp, lax.rem(i, tp))
        pl.semaphore_signal(
            barrier, inc=1, device_id=to(z2, t2), device_id_type=pl.DeviceIdType.MESH
        )
        return c

    lax.fori_loop(1, n, greet, 0)

    loads = [
        pltpu.make_async_copy(src, dst, w_sem.at[i])
        for i, (src, dst) in enumerate(
            ((wg_hbm.at[0], wg), (wu_hbm.at[0], wu), (wd_hbm.at[0], wd), (wo_hbm, wo))
        )
    ]
    for load in loads:
        load.start()

    x = tok_ref[...].astype(F32)
    centre = jnp.mean(x, axis=1, keepdims=True)
    spread = jnp.mean(jnp.square(x - centre), axis=1, keepdims=True)
    normed = ((x - centre) * lax.rsqrt(spread + layer_eps) * egain_ref[...]).astype(BF16)
    tok_r = lax.broadcasted_iota(jnp.int32, (tokens, tokens), 0)
    tok_c = lax.broadcasted_iota(jnp.int32, (tokens, tokens), 1)

    def column(row):
        return jnp.sum(jnp.where(tok_r == tok_c, row, 0.0), axis=1, keepdims=True)

    top = routes_ref.shape[0]
    routes = [column(routes_ref[i : i + 1, :].astype(F32)).astype(jnp.int32) for i in range(top)]
    lanes = max(128, -(-n // 128) * 128)
    lane_e = lax.broadcasted_iota(jnp.int32, (tokens, lanes), 1)
    hots = [(lane_e == routes[i]).astype(F32) for i in range(top)]
    earlier = dot((tok_r > tok_c).astype(F32).astype(BF16), sum(hots).astype(BF16))
    slot_i = lax.broadcasted_iota(jnp.int32, (tokens, n * stride), 1)
    pick = jnp.zeros((tokens, n * stride), F32)
    weigh = jnp.zeros((tokens, n * stride), F32)
    for i in range(top):
        place = jnp.sum(earlier * hots[i], axis=1, keepdims=True).astype(jnp.int32)
        mine = (slot_i == routes[i] * stride + place).astype(F32)
        pick = pick + mine
        weigh = weigh + mine * column(rw_ref[i : i + 1, :])
    comb[...] = weigh
    pick = pick.astype(BF16)
    out_rows[...] = dot(pick, normed, ((0,), (0,))).astype(BF16)

    pl.semaphore_wait(barrier, n - 1)

    def rows_of(ref, index):
        return ref.at[pl.ds(pl.multiple_of(index * stride, row_tile), stride)]

    def exchange(src, dst, send, recv, z2, t2, arriving):
        p = z2 * tp + t2
        return pltpu.make_async_remote_copy(
            src_ref=rows_of(src, p),
            dst_ref=rows_of(dst, p if arriving else me),
            send_sem=send.at[p],
            recv_sem=recv.at[p if arriving else me],
            device_id=to(z2, t2),
            device_id_type=pl.DeviceIdType.MESH,
        )

    def dispatch(z2, t2, arriving=False):
        return exchange(out_rows, arrived, d_send, d_recv, z2, t2, arriving)

    def give_back(z2, t2, arriving=False):
        return exchange(results, returned, r_send, r_recv, z2, t2, arriving)

    def each_peer(first, action, last=n):
        def turn(i, c):
            z2, t2 = peer(i // tp, lax.rem(i, tp))
            action(z2, t2)
            return c

        lax.fori_loop(first, last, turn, 0)

    own = pl.ds(pl.multiple_of(me * stride, row_tile), stride)

    def chain(index, src, dst, z2):
        return pltpu.make_async_remote_copy(
            src_ref=src,
            dst_ref=dst,
            send_sem=c_send.at[index],
            recv_sem=c_recv.at[index],
            device_id=to(z2, t),
            device_id_type=pl.DeviceIdType.MESH,
        )

    each_peer(1, lambda z2, t2: dispatch(z2, t2).start(), 2 * tp)

    rows_i = lax.broadcasted_iota(jnp.int32, (span, span), 0)
    cols_i = lax.broadcasted_iota(jnp.int32, (span, span), 1)
    lower = rows_i >= cols_i
    upper = rows_i <= cols_i
    diag = rows_i == cols_i

    fg = fg_ref[...]
    lf_row = jnp.minimum(fg, 0.0) - jnp.log1p(jnp.exp(-jnp.abs(fg))) + xf_ref[...]
    in_row = ig_ref[...]
    lf_col = jnp.sum(jnp.where(diag, lf_row, 0.0), axis=1, keepdims=True)
    in_col = jnp.sum(jnp.where(diag, in_row, 0.0), axis=1, keepdims=True)
    through_col = jnp.sum(jnp.where(lower, lf_row, 0.0), axis=1, keepdims=True)
    through_row = jnp.sum(jnp.where(upper, lf_col, 0.0), axis=0, keepdims=True)
    before_col = through_col - lf_col
    before_row = through_row - lf_row
    total = jnp.sum(lf_row, axis=1, keepdims=True)

    keys = k_ref[...]
    values = v_ref[...]
    keys_f32 = keys.astype(F32)
    fw_w = total - through_col + in_col
    bw_w = before_col + in_col
    fw_top = jnp.max(fw_w, axis=0, keepdims=True)
    bw_top = jnp.max(bw_w, axis=0, keepdims=True)
    fw_own[...] = dot((keys_f32 * jnp.exp(fw_w - fw_top)).astype(BF16), values, ((0,), (0,)))
    bw_own[...] = dot((keys_f32 * jnp.exp(bw_w - bw_top)).astype(BF16), values, ((0,), (0,)))

    after = lax.rem(z + 1, ep)
    ahead = lax.rem(z + ep - 1, ep)
    fw_chain = (chain(0, fw_top_out, fw_top_in, after), chain(1, fw_out, fw_in, after))
    bw_chain = (chain(2, bw_top_out, bw_top_in, ahead), chain(3, bw_out, bw_in, ahead))

    @pl.when(z == 0)
    def _():
        fw_in[...] = jnp.zeros_like(fw_in)
        fw_top_in[...] = jnp.full_like(fw_top_in, lowest_log)

    @pl.when(z == ep - 1)
    def _():
        bw_in[...] = jnp.zeros_like(bw_in)
        bw_top_in[...] = jnp.full_like(bw_top_in, lowest_log)

    def pass_on(copies, in_ref, top_in, own_ref, own_top, out_ref, top_out):
        shifted = total + top_in[0:1, 0:1]
        joined = jnp.maximum(shifted, own_top)
        out_ref[...] = (
            jnp.exp(shifted - joined) * in_ref[...].astype(F32)
            + jnp.exp(own_top - joined) * own_ref[...]
        ).astype(BF16)
        top_out[...] = jnp.broadcast_to(joined, top_out.shape)
        for copy in copies:
            copy.start()

    def stage(s, c):
        @pl.when(z == s)
        def _():
            @pl.when(z > 0)
            def _():
                for copy in fw_chain:
                    copy.wait_recv()

            pass_on(fw_chain, fw_in, fw_top_in, fw_own, fw_top, fw_out, fw_top_out)

        @pl.when(ep - 1 - z == s)
        def _():
            @pl.when(z < ep - 1)
            def _():
                for copy in bw_chain:
                    copy.wait_recv()

            pass_on(bw_chain, bw_in, bw_top_in, bw_own, bw_top, bw_out, bw_top_out)
        return c

    lax.fori_loop(0, 1, stage, 0)
    each_peer(2 * tp, lambda z2, t2: dispatch(z2, t2).start())
    arrived[own] = out_rows[own]

    fe = wg.shape[1]
    cols = 256
    plane_rows = tp * stride
    for load in loads[:3]:
        load.wait()

    def expert_group(g):
        first, last = max(1, 2 * g * tp), 2 * (g + 1) * tp
        each_peer(first, lambda z2, t2: dispatch(z2, t2, True).wait_recv(), last)
        near_at, far_at = [
            pl.ds(pl.multiple_of(lax.rem(z + 2 * g + i, ep) * plane_rows, row_tile), plane_rows)
            for i in range(2)
        ]

        def up(j, c2):
            f = pl.ds(pl.multiple_of(j * cols, cols), cols)
            rows = jnp.concatenate([arrived[near_at, :], arrived[far_at, :]], axis=0)
            gate_part = dot(rows, wg[:, f])
            up_part = dot(rows, wu[:, f])
            hidden[:, f] = (gate_part * jax.nn.sigmoid(gate_part) * up_part).astype(BF16)
            return c2

        lax.fori_loop(0, fe // cols, up, 0)

        def down(j, c2):
            f = pl.ds(pl.multiple_of(j * cols, cols), cols)
            made = dot(hidden[...], wd[:, f]).astype(BF16)
            results[near_at, f] = made[:plane_rows]
            results[far_at, f] = made[plane_rows:]
            return c2

        lax.fori_loop(0, width // cols, down, 0)
        each_peer(first, lambda z2, t2: give_back(z2, t2).start(), last)

    groups = ep // 2
    for g in range(groups):
        lax.fori_loop(1 + g * (ep - 2) // groups, 1 + (g + 1) * (ep - 2) // groups, stage, 0)
        expert_group(g)
    returned[own] = results[own]

    from_row = through_col - through_row + in_row
    fw_log = jnp.where(lower, from_row, -jnp.inf)
    bw_log = jnp.where(upper, before_row - before_col + in_row, -jnp.inf)
    inner_top = jnp.maximum(
        jnp.max(fw_log, axis=1, keepdims=True), jnp.max(bw_log, axis=1, keepdims=True)
    )

    @pl.when(z == ep - 1)
    def _():
        for copy in fw_chain:
            copy.wait_recv()

    @pl.when(z == 0)
    def _():
        for copy in bw_chain:
            copy.wait_recv()

    from_prior = through_col + fw_top_in[0:1, 0:1]
    from_later = total - before_col + bw_top_in[0:1, 0:1]
    row_top = jnp.maximum(inner_top, jnp.maximum(from_prior, from_later))
    weights = jnp.exp(fw_log - row_top) + jnp.exp(bw_log - row_top)
    queries = q_ref[...]
    scale = queries.shape[1] ** (-0.5)
    scores = dot(queries, keys, ((1,), (1,))) * scale
    near = (scores * weights).astype(BF16)
    carried = jnp.exp(from_prior - row_top) * dot(queries, fw_in[...])
    carried = carried + jnp.exp(from_later - row_top) * dot(queries, bw_in[...])
    head_rows = dot(near, values) + carried * scale
    mean_square = jnp.mean(head_rows * head_rows, axis=1, keepdims=True)
    normed_rows = head_rows * lax.rsqrt(mean_square + norm_eps) * hgain_ref[...]
    gated[...] = (jax.nn.sigmoid(og_ref[...].astype(F32)) * normed_rows).astype(BF16)

    loads[3].wait()

    def project(i, c):
        at = pl.ds(pl.multiple_of(i * cols, cols), cols)
        parts_out[:, at] = dot(gated[...], wo[:, at]).astype(BF16)
        return c

    lax.fori_loop(0, width // cols, project, 0)

    def share(dt, arriving=False):
        t2 = lax.rem(t + dt, tp)
        slot = t2 if arriving else t
        return pltpu.make_async_remote_copy(
            src_ref=parts_out.at[pl.ds(pl.multiple_of(t2 * sub, row_tile), sub)],
            dst_ref=parts_in.at[slot],
            send_sem=p_send.at[t2],
            recv_sem=p_recv.at[slot],
            device_id=to(z, t2),
            device_id_type=pl.DeviceIdType.MESH,
        )

    for dt in range(1, tp):
        share(dt).start()
    parts_in[t] = parts_out[pl.ds(pl.multiple_of(t * sub, row_tile), sub), :]

    for dt in range(1, tp):
        share(dt, True).wait_recv()
    mixed = parts_in[0].astype(F32)
    for i in range(1, tp):
        mixed = mixed + parts_in[i].astype(F32)
    mix_ref[...] = mixed.astype(BF16)

    weigh = comb[...]
    high = weigh.astype(BF16)
    low = (weigh - high.astype(F32)).astype(BF16)
    each_peer(1, lambda z2, t2: give_back(z2, t2, True).wait_recv())
    for j in range(width // cols):
        f = slice(j * cols, (j + 1) * cols)
        rows = returned[:, f]
        exp_ref[:, f] = (dot(high, rows) + dot(low, rows)).astype(BF16)

    @pl.when(z < ep - 1)
    def _():
        for copy in fw_chain:
            copy.wait_send()

    @pl.when(z > 0)
    def _():
        for copy in bw_chain:
            copy.wait_send()

    for dt in range(1, tp):
        share(dt).wait_send()
    each_peer(1, lambda z2, t2: dispatch(z2, t2).wait_send())
    each_peer(1, lambda z2, t2: give_back(z2, t2).wait_send())


def body(
    queries,
    head_key_rows,
    head_value_rows,
    output_gate_logits,
    log_input_gate,
    forget_gate_logits,
    extra_log_forget,
    head_norm_gain,
    memory_output_matrix,
    expert_input_tokens,
    expert_norm_gain,
    routes,
    routed_expert_weight,
    expert_gate_matrix,
    expert_up_matrix,
    expert_down_matrix,
):
    ep = lax.axis_size("ep")
    tp = lax.axis_size("tp")
    n = ep * tp
    span, dqk = queries.shape
    dv = head_value_rows.shape[1]
    tokens, width = expert_input_tokens.shape
    fe = expert_gate_matrix.shape[2]
    capacity = max(2, 2 * tokens * routes.shape[1] // n)
    stride = -(-capacity // row_tile) * row_tile
    slots = n * stride
    vmem = pl.BlockSpec(memory_space=pltpu.VMEM)
    hbm = pl.BlockSpec(memory_space=pl.ANY)
    dma = pltpu.SemaphoreType.DMA
    return pl.pallas_call(
        functools.partial(step_kernel, ep, tp, stride, capacity),
        out_shape=(
            jax.ShapeDtypeStruct((span // tp, width), BF16),
            jax.ShapeDtypeStruct((tokens, width), BF16),
        ),
        in_specs=[vmem] * 8 + [hbm] + [vmem] * 4 + [hbm] * 3,
        out_specs=(vmem, vmem),
        scratch_shapes=[
            pltpu.VMEM((dv, width), BF16),
            pltpu.VMEM((width, fe), BF16),
            pltpu.VMEM((width, fe), BF16),
            pltpu.VMEM((fe, width), BF16),
            pltpu.VMEM((slots, width), BF16),
            pltpu.VMEM((slots, width), BF16),
            pltpu.VMEM((slots, width), BF16),
            pltpu.VMEM((slots, width), BF16),
            pltpu.VMEM((tokens, slots), F32),
            pltpu.VMEM((dqk, dv), F32),
            pltpu.VMEM((dqk, dv), F32),
            pltpu.VMEM((dqk, dv), BF16),
            pltpu.VMEM((dqk, dv), BF16),
            pltpu.VMEM((dqk, dv), BF16),
            pltpu.VMEM((dqk, dv), BF16),
            pltpu.VMEM((8, 128), F32),
            pltpu.VMEM((8, 128), F32),
            pltpu.VMEM((8, 128), F32),
            pltpu.VMEM((8, 128), F32),
            pltpu.VMEM((span, width), BF16),
            pltpu.VMEM((tp, span // tp, width), BF16),
            pltpu.VMEM((span, dv), BF16),
            pltpu.VMEM((2 * tp * stride, fe), BF16),
            dma((4,)),
            dma((n,)),
            dma((n,)),
            dma((n,)),
            dma((n,)),
            dma((4,)),
            dma((4,)),
            dma((tp,)),
            dma((tp,)),
        ],
        compiler_params=pltpu.CompilerParams(
            collective_id=0, has_side_effects=True, vmem_limit_bytes=64 * 1024 * 1024 - 65536
        ),
    )(
        queries,
        head_key_rows,
        head_value_rows,
        output_gate_logits,
        log_input_gate,
        forget_gate_logits,
        extra_log_forget,
        head_norm_gain[None, :],
        memory_output_matrix,
        expert_input_tokens,
        expert_norm_gain[None, :],
        routes.T,
        routed_expert_weight.T,
        expert_gate_matrix,
        expert_up_matrix,
        expert_down_matrix,
    )


def solution(mesh):
    in_specs = (
        P(("grp", "ep"), "tp"),
        P(("grp", "ep"), "tp"),
        P(("grp", "ep"), "tp"),
        P(("grp", "ep"), "tp"),
        P("tp", ("grp", "ep")),
        P("tp", ("grp", "ep")),
        P("tp", ("grp", "ep")),
        P("tp"),
        P("tp", None),
        P(("grp", "ep", "tp"), None),
        P(),
        P(("grp", "ep", "tp"), None),
        P(("grp", "ep", "tp"), None),
        P(("ep", "tp"), None, None),
        P(("ep", "tp"), None, None),
        P(("ep", "tp"), None, None),
    )
    out_specs = (P(("grp", "ep", "tp"), None), P(("grp", "ep", "tp"), None))
    return jax.shard_map(body, mesh=mesh, in_specs=in_specs, out_specs=out_specs, check_vma=False)
```

```python
import functools

import jax
import jax.numpy as jnp
from jax import lax
from jax.experimental import pallas as pl
from jax.experimental.pallas import tpu as pltpu
from jax.sharding import PartitionSpec as P

lowest_log = -1e30
norm_eps = 1e-06
layer_eps = 1e-05
row_tile = 16

F32 = jnp.float32
BF16 = jnp.bfloat16


def dot(a, b, contract=((1,), (0,))):
    return lax.dot_general(a, b, (contract, ((), ())), preferred_element_type=F32)


def step_kernel(
    ep,
    tp,
    stride,
    capacity,
    q_ref,
    k_ref,
    v_ref,
    og_ref,
    ig_ref,
    fg_ref,
    xf_ref,
    hgain_ref,
    wo_hbm,
    tok_ref,
    egain_ref,
    routes_ref,
    rw_ref,
    wg_hbm,
    wu_hbm,
    wd_hbm,
    out_ref,
    wo,
    wg,
    wu,
    wd,
    out_rows,
    arrived,
    results,
    returned,
    comb,
    fw_own,
    bw_own,
    fw_in,
    bw_in,
    fw_out,
    bw_out,
    fw_top_in,
    bw_top_in,
    fw_top_out,
    bw_top_out,
    parts_out,
    parts_in,
    gated,
    hidden,
    w_sem,
    d_send,
    d_recv,
    r_send,
    r_recv,
    c_send,
    c_recv,
    p_send,
    p_recv,
):
    n = ep * tp
    z = lax.axis_index("ep")
    t = lax.axis_index("tp")
    me = z * tp + t
    span = q_ref.shape[0]
    tokens, width = tok_ref.shape
    sub = span // tp

    def peer(dz, dt):
        return lax.rem(z + dz, ep), lax.rem(t + dt, tp)

    def to(z2, t2):
        return {"ep": z2, "tp": t2}

    barrier = pltpu.get_barrier_semaphore()

    def greet(i, c):
        z2, t2 = peer(i // tp, lax.rem(i, tp))
        pl.semaphore_signal(
            barrier, inc=1, device_id=to(z2, t2), device_id_type=pl.DeviceIdType.MESH
        )
        return c

    lax.fori_loop(1, n, greet, 0)

    loads = [
        pltpu.make_async_copy(src, dst, w_sem.at[i])
        for i, (src, dst) in enumerate(
            ((wg_hbm.at[0], wg), (wu_hbm.at[0], wu), (wd_hbm.at[0], wd), (wo_hbm, wo))
        )
    ]
    for load in loads:
        load.start()

    x = tok_ref[...].astype(F32)
    centre = jnp.mean(x, axis=1, keepdims=True)
    spread = jnp.mean(jnp.square(x - centre), axis=1, keepdims=True)
    normed = ((x - centre) * lax.rsqrt(spread + layer_eps) * egain_ref[...]).astype(BF16)
    tok_r = lax.broadcasted_iota(jnp.int32, (tokens, tokens), 0)
    tok_c = lax.broadcasted_iota(jnp.int32, (tokens, tokens), 1)

    def column(row):
        return jnp.sum(jnp.where(tok_r == tok_c, row, 0.0), axis=1, keepdims=True)

    top = routes_ref.shape[0]
    routes = [column(routes_ref[i : i + 1, :].astype(F32)).astype(jnp.int32) for i in range(top)]
    lanes = max(128, -(-n // 128) * 128)
    lane_e = lax.broadcasted_iota(jnp.int32, (tokens, lanes), 1)
    hots = [(lane_e == routes[i]).astype(F32) for i in range(top)]
    earlier = dot((tok_r > tok_c).astype(F32).astype(BF16), sum(hots).astype(BF16))
    slot_i = lax.broadcasted_iota(jnp.int32, (tokens, n * stride), 1)
    pick = jnp.zeros((tokens, n * stride), F32)
    weigh = jnp.zeros((tokens, n * stride), F32)
    for i in range(top):
        place = jnp.sum(earlier * hots[i], axis=1, keepdims=True).astype(jnp.int32)
        mine = (slot_i == routes[i] * stride + place).astype(F32)
        pick = pick + mine
        weigh = weigh + mine * column(rw_ref[i : i + 1, :])
    comb[...] = weigh
    pick = pick.astype(BF16)
    out_rows[...] = dot(pick, normed, ((0,), (0,))).astype(BF16)

    pl.semaphore_wait(barrier, n - 1)

    def rows_of(ref, index):
        return ref.at[pl.ds(pl.multiple_of(index * stride, row_tile), stride)]

    def exchange(src, dst, send, recv, z2, t2, arriving):
        p = z2 * tp + t2
        return pltpu.make_async_remote_copy(
            src_ref=rows_of(src, p),
            dst_ref=rows_of(dst, p if arriving else me),
            send_sem=send.at[p],
            recv_sem=recv.at[p if arriving else me],
            device_id=to(z2, t2),
            device_id_type=pl.DeviceIdType.MESH,
        )

    def dispatch(z2, t2, arriving=False):
        return exchange(out_rows, arrived, d_send, d_recv, z2, t2, arriving)

    def give_back(z2, t2, arriving=False):
        return exchange(results, returned, r_send, r_recv, z2, t2, arriving)

    def each_peer(first, action, last=n):
        def turn(i, c):
            z2, t2 = peer(i // tp, lax.rem(i, tp))
            action(z2, t2)
            return c

        lax.fori_loop(first, last, turn, 0)

    own = pl.ds(pl.multiple_of(me * stride, row_tile), stride)

    def chain(index, src, dst, z2):
        return pltpu.make_async_remote_copy(
            src_ref=src,
            dst_ref=dst,
            send_sem=c_send.at[index],
            recv_sem=c_recv.at[index],
            device_id=to(z2, t),
            device_id_type=pl.DeviceIdType.MESH,
        )

    each_peer(1, lambda z2, t2: dispatch(z2, t2).start(), 2 * tp)

    rows_i = lax.broadcasted_iota(jnp.int32, (span, span), 0)
    cols_i = lax.broadcasted_iota(jnp.int32, (span, span), 1)
    lower = rows_i >= cols_i
    upper = rows_i <= cols_i
    diag = rows_i == cols_i

    fg = fg_ref[...]
    lf_row = jnp.minimum(fg, 0.0) - jnp.log1p(jnp.exp(-jnp.abs(fg))) + xf_ref[...]
    in_row = ig_ref[...]
    lf_col = jnp.sum(jnp.where(diag, lf_row, 0.0), axis=1, keepdims=True)
    in_col = jnp.sum(jnp.where(diag, in_row, 0.0), axis=1, keepdims=True)
    through_col = jnp.sum(jnp.where(lower, lf_row, 0.0), axis=1, keepdims=True)
    through_row = jnp.sum(jnp.where(upper, lf_col, 0.0), axis=0, keepdims=True)
    before_col = through_col - lf_col
    before_row = through_row - lf_row
    total = jnp.sum(lf_row, axis=1, keepdims=True)

    keys = k_ref[...]
    values = v_ref[...]
    keys_f32 = keys.astype(F32)
    fw_w = total - through_col + in_col
    bw_w = before_col + in_col
    fw_top = jnp.max(fw_w, axis=0, keepdims=True)
    bw_top = jnp.max(bw_w, axis=0, keepdims=True)
    fw_own[...] = dot((keys_f32 * jnp.exp(fw_w - fw_top)).astype(BF16), values, ((0,), (0,)))
    bw_own[...] = dot((keys_f32 * jnp.exp(bw_w - bw_top)).astype(BF16), values, ((0,), (0,)))

    after = lax.rem(z + 1, ep)
    ahead = lax.rem(z + ep - 1, ep)
    fw_chain = (chain(0, fw_top_out, fw_top_in, after), chain(1, fw_out, fw_in, after))
    bw_chain = (chain(2, bw_top_out, bw_top_in, ahead), chain(3, bw_out, bw_in, ahead))

    @pl.when(z == 0)
    def _():
        fw_in[...] = jnp.zeros_like(fw_in)
        fw_top_in[...] = jnp.full_like(fw_top_in, lowest_log)

    @pl.when(z == ep - 1)
    def _():
        bw_in[...] = jnp.zeros_like(bw_in)
        bw_top_in[...] = jnp.full_like(bw_top_in, lowest_log)

    def pass_on(copies, in_ref, top_in, own_ref, own_top, out_ref, top_out):
        shifted = total + top_in[0:1, 0:1]
        joined = jnp.maximum(shifted, own_top)
        out_ref[...] = (
            jnp.exp(shifted - joined) * in_ref[...].astype(F32)
            + jnp.exp(own_top - joined) * own_ref[...]
        ).astype(BF16)
        top_out[...] = jnp.broadcast_to(joined, top_out.shape)
        for copy in copies:
            copy.start()

    def stage(s, c):
        @pl.when(z == s)
        def _():
            @pl.when(z > 0)
            def _():
                for copy in fw_chain:
                    copy.wait_recv()

            pass_on(fw_chain, fw_in, fw_top_in, fw_own, fw_top, fw_out, fw_top_out)

        @pl.when(ep - 1 - z == s)
        def _():
            @pl.when(z < ep - 1)
            def _():
                for copy in bw_chain:
                    copy.wait_recv()

            pass_on(bw_chain, bw_in, bw_top_in, bw_own, bw_top, bw_out, bw_top_out)
        return c

    lax.fori_loop(0, 1, stage, 0)
    each_peer(2 * tp, lambda z2, t2: dispatch(z2, t2).start())
    arrived[own] = out_rows[own]

    fe = wg.shape[1]
    cols = 512
    plane_rows = tp * stride
    for load in loads[:3]:
        load.wait()

    def expert_group(g):
        first, last = max(1, 2 * g * tp), 2 * (g + 1) * tp
        each_peer(first, lambda z2, t2: dispatch(z2, t2, True).wait_recv(), last)
        near_at, far_at = [
            pl.ds(pl.multiple_of(lax.rem(z + 2 * g + i, ep) * plane_rows, row_tile), plane_rows)
            for i in range(2)
        ]

        def up(j, c2):
            f = pl.ds(pl.multiple_of(j * cols, cols), cols)
            rows = jnp.concatenate([arrived[near_at, :], arrived[far_at, :]], axis=0)
            gate_part = dot(rows, wg[:, f])
            up_part = dot(rows, wu[:, f])
            hidden[:, f] = (gate_part * jax.nn.sigmoid(gate_part) * up_part).astype(BF16)
            return c2

        lax.fori_loop(0, fe // cols, up, 0)

        def down(j, c2):
            f = pl.ds(pl.multiple_of(j * cols, cols), cols)
            made = dot(hidden[...], wd[:, f]).astype(BF16)
            results[near_at, f] = made[:plane_rows]
            results[far_at, f] = made[plane_rows:]
            return c2

        lax.fori_loop(0, width // cols, down, 0)
        each_peer(first, lambda z2, t2: give_back(z2, t2).start(), last)

    groups = ep // 2
    for g in range(groups):
        lax.fori_loop(1 + g * (ep - 2) // groups, 1 + (g + 1) * (ep - 2) // groups, stage, 0)
        expert_group(g)
    returned[own] = results[own]

    from_row = through_col - through_row + in_row
    fw_log = jnp.where(lower, from_row, -jnp.inf)
    bw_log = jnp.where(upper, before_row - before_col + in_row, -jnp.inf)
    inner_top = jnp.maximum(
        jnp.max(fw_log, axis=1, keepdims=True), jnp.max(bw_log, axis=1, keepdims=True)
    )

    @pl.when(z == ep - 1)
    def _():
        for copy in fw_chain:
            copy.wait_recv()

    @pl.when(z == 0)
    def _():
        for copy in bw_chain:
            copy.wait_recv()

    from_prior = through_col + fw_top_in[0:1, 0:1]
    from_later = total - before_col + bw_top_in[0:1, 0:1]
    row_top = jnp.maximum(inner_top, jnp.maximum(from_prior, from_later))
    weights = jnp.exp(fw_log - row_top) + jnp.exp(bw_log - row_top)
    queries = q_ref[...]
    scale = queries.shape[1] ** (-0.5)
    scores = dot(queries, keys, ((1,), (1,))) * scale
    near = (scores * weights).astype(BF16)
    carried = jnp.exp(from_prior - row_top) * dot(queries, fw_in[...])
    carried = carried + jnp.exp(from_later - row_top) * dot(queries, bw_in[...])
    head_rows = dot(near, values) + carried * scale
    mean_square = jnp.mean(head_rows * head_rows, axis=1, keepdims=True)
    normed_rows = head_rows * lax.rsqrt(mean_square + norm_eps) * hgain_ref[...]
    gated[...] = (jax.nn.sigmoid(og_ref[...].astype(F32)) * normed_rows).astype(BF16)

    loads[3].wait()

    def project(i, c):
        at = pl.ds(pl.multiple_of(i * cols, cols), cols)
        parts_out[:, at] = dot(gated[...], wo[:, at]).astype(BF16)
        return c

    lax.fori_loop(0, width // cols, project, 0)

    def share(dt, arriving=False):
        t2 = lax.rem(t + dt, tp)
        slot = t2 if arriving else t
        return pltpu.make_async_remote_copy(
            src_ref=parts_out.at[pl.ds(pl.multiple_of(t2 * sub, row_tile), sub)],
            dst_ref=parts_in.at[slot],
            send_sem=p_send.at[t2],
            recv_sem=p_recv.at[slot],
            device_id=to(z, t2),
            device_id_type=pl.DeviceIdType.MESH,
        )

    for dt in range(1, tp):
        share(dt).start()
    parts_in[t] = parts_out[pl.ds(pl.multiple_of(t * sub, row_tile), sub), :]

    for dt in range(1, tp):
        share(dt, True).wait_recv()
    mixed = parts_in[0].astype(F32)
    for i in range(1, tp):
        mixed = mixed + parts_in[i].astype(F32)
    out_ref[0:sub, :] = mixed.astype(BF16)

    weigh = comb[...]
    high = weigh.astype(BF16)
    low = (weigh - high.astype(F32)).astype(BF16)
    each_peer(1, lambda z2, t2: give_back(z2, t2, True).wait_recv())
    for j in range(width // cols):
        f = slice(j * cols, (j + 1) * cols)
        rows = returned[:, f]
        out_ref[sub : sub + tokens, f] = (dot(high, rows) + dot(low, rows)).astype(BF16)

    @pl.when(z < ep - 1)
    def _():
        for copy in fw_chain:
            copy.wait_send()

    @pl.when(z > 0)
    def _():
        for copy in bw_chain:
            copy.wait_send()

    for dt in range(1, tp):
        share(dt).wait_send()
    each_peer(1, lambda z2, t2: dispatch(z2, t2).wait_send())
    each_peer(1, lambda z2, t2: give_back(z2, t2).wait_send())


def body(
    queries,
    head_key_rows,
    head_value_rows,
    output_gate_logits,
    log_input_gate,
    forget_gate_logits,
    extra_log_forget,
    head_norm_gain,
    memory_output_matrix,
    expert_input_tokens,
    expert_norm_gain,
    routes,
    routed_expert_weight,
    expert_gate_matrix,
    expert_up_matrix,
    expert_down_matrix,
):
    ep = lax.axis_size("ep")
    tp = lax.axis_size("tp")
    n = ep * tp
    span, dqk = queries.shape
    dv = head_value_rows.shape[1]
    tokens, width = expert_input_tokens.shape
    fe = expert_gate_matrix.shape[2]
    capacity = max(2, 2 * tokens * routes.shape[1] // n)
    stride = -(-capacity // row_tile) * row_tile
    slots = n * stride
    vmem = pl.BlockSpec(memory_space=pltpu.VMEM)
    hbm = pl.BlockSpec(memory_space=pl.ANY)
    dma = pltpu.SemaphoreType.DMA
    both = pl.pallas_call(
        functools.partial(step_kernel, ep, tp, stride, capacity),
        out_shape=jax.ShapeDtypeStruct((span // tp + tokens, width), BF16),
        in_specs=[vmem] * 8 + [hbm] + [vmem] * 4 + [hbm] * 3,
        out_specs=vmem,
        scratch_shapes=[
            pltpu.VMEM((dv, width), BF16),
            pltpu.VMEM((width, fe), BF16),
            pltpu.VMEM((width, fe), BF16),
            pltpu.VMEM((fe, width), BF16),
            pltpu.VMEM((slots, width), BF16),
            pltpu.VMEM((slots, width), BF16),
            pltpu.VMEM((slots, width), BF16),
            pltpu.VMEM((slots, width), BF16),
            pltpu.VMEM((tokens, slots), F32),
            pltpu.VMEM((dqk, dv), F32),
            pltpu.VMEM((dqk, dv), F32),
            pltpu.VMEM((dqk, dv), BF16),
            pltpu.VMEM((dqk, dv), BF16),
            pltpu.VMEM((dqk, dv), BF16),
            pltpu.VMEM((dqk, dv), BF16),
            pltpu.VMEM((8, 128), F32),
            pltpu.VMEM((8, 128), F32),
            pltpu.VMEM((8, 128), F32),
            pltpu.VMEM((8, 128), F32),
            pltpu.VMEM((span, width), BF16),
            pltpu.VMEM((tp, span // tp, width), BF16),
            pltpu.VMEM((span, dv), BF16),
            pltpu.VMEM((2 * tp * stride, fe), BF16),
            dma((4,)),
            dma((n,)),
            dma((n,)),
            dma((n,)),
            dma((n,)),
            dma((4,)),
            dma((4,)),
            dma((tp,)),
            dma((tp,)),
        ],
        compiler_params=pltpu.CompilerParams(
            collective_id=0, has_side_effects=True, vmem_limit_bytes=64 * 1024 * 1024 - 65536
        ),
    )(
        queries,
        head_key_rows,
        head_value_rows,
        output_gate_logits,
        log_input_gate,
        forget_gate_logits,
        extra_log_forget,
        head_norm_gain[None, :],
        memory_output_matrix,
        expert_input_tokens,
        expert_norm_gain[None, :],
        routes.T,
        routed_expert_weight.T,
        expert_gate_matrix,
        expert_up_matrix,
        expert_down_matrix,
    )
    return both[: span // tp], both[span // tp :]


def solution(mesh):
    in_specs = (
        P(("grp", "ep"), "tp"),
        P(("grp", "ep"), "tp"),
        P(("grp", "ep"), "tp"),
        P(("grp", "ep"), "tp"),
        P("tp", ("grp", "ep")),
        P("tp", ("grp", "ep")),
        P("tp", ("grp", "ep")),
        P("tp"),
        P("tp", None),
        P(("grp", "ep", "tp"), None),
        P(),
        P(("grp", "ep", "tp"), None),
        P(("grp", "ep", "tp"), None),
        P(("ep", "tp"), None, None),
        P(("ep", "tp"), None, None),
        P(("ep", "tp"), None, None),
    )
    out_specs = (P(("grp", "ep", "tp"), None), P(("grp", "ep", "tp"), None))
    return jax.shard_map(body, mesh=mesh, in_specs=in_specs, out_specs=out_specs, check_vma=False)
```
